32 devices in a mesh: sp: 4 (over z), fs: 4 (over y, x), tp: 2 (over core).
Axes of the slice: x: 2, y: 2, z: 4, core: 2. Of those that a mesh axis runs over, the one named last changes fastest.
Arguments:
- tokens: bfloat16 [2048, 2048], P(('fs', 'sp'), 'tp'), parts along dimension 0, may hold values from -6 to 6
- norm_gain: float32 [2048], replicated, may hold values from 0.1 to 1.9
- w_recur_in: bfloat16 [2048, 1024], P(None, 'tp'), may hold values from -0.125 to 0.125
- conv_weight: float32 [4, 1024], P(None, 'tp'), may hold values from -3 to 3
- w_gate_decay: bfloat16 [16, 64, 64], P('tp'), may hold values from -0.75 to 0.75
- w_gate_input: bfloat16 [16, 64, 64], P('tp'), may hold values from -0.75 to 0.75
- decay_base: float32 [1024], P('tp'), may hold values from 0 to 0.01, as said below
- extra_decay: float32 [2048, 16], P(('fs', 'sp'), 'tp'), parts along dimension 0, may hold values from 0 to 1, as said below
- w_query: bfloat16 [2048, 1024], P(None, 'tp'), may hold values from -1 to 1
- w_key: bfloat16 [2048, 256], P(None, 'tp'), may hold values from -20 to 20
- w_value: bfloat16 [2048, 256], P(None, 'tp'), may hold values from -0.125 to 0.125
- mix_lambda: float32 [8], P('tp'), may hold values from 0.3 to 0.8
- head_gain: float32 [128], replicated, may hold values from 0.1 to 1.9
- w_out_recur: bfloat16 [1024, 2048], P('tp'), may hold values from -0.125 to 0.125
- w_out_attend: bfloat16 [1024, 2048], P('tp'), may hold values from -0.125 to 0.125
- out_gain: float32 [2048], replicated, may hold values from 0.1 to 1.9
Outputs:
- mixed: bfloat16 [2048, 2048], P(('fs', 'sp', 'tp')), parts along dimension 0
The draws below stay inside these ranges and needn't reach their ends.
There are 4 independent parts, one for each index of `fs`. The reference program is written for one: setup_inputs(seed, part) draws one part's arguments, and reference() takes and returns one part's arrays. A program takes and returns all parts, laid end to end along the dimension named above; an argument that names none is the same for every part. Nothing has to cross between parts.
Inputs may be any that keep to these rules, and one draw needn't show every extreme that they name: `decay_base`: positive rates of each channel. `extra_decay`: non-negative added log-decays.
All inputs are finite; a program needn't handle non-finite values.
Results may differ from the reference program's by a relative error of at most 0.012.
The reference program's roundings to bfloat16 on the way (of `scaled`, `conv_in`, `recur_out` and `attend_out`) count: a program that leaves them out, or rounds other values in their place, can miss the bound.
Values may be sent and summed in bfloat16 or wider, within the bound.
A program may use at most 128 MiB of HBM per device.

```python
import math
import jax
import jax.numpy as jnp
from jax import lax

D = 2048
HEAD = 64
RECURRENT_HEADS = 16
CONV = 4
DA_HEADS = 8
KV_HEADS = 2
TOK_DEV = 128
RG_W = 1024
DV = 128
SEQUENCE_TOKENS = 512


def draw_decay_base(key, part):
    slow_key, fast_key, pick_key = jax.random.split(jax.random.fold_in(key, 11), 3)
    slow_rate = jax.random.uniform(slow_key, (RG_W,), jnp.float32, 0.05, 0.15) / SEQUENCE_TOKENS
    fast_rate = jnp.exp(jax.random.uniform(fast_key, (RG_W,), jnp.float32, math.log(0.0025), math.log(0.0083)))
    fast_share = 0.5
    chosen = jax.random.uniform(pick_key, (RG_W,), jnp.float32) < fast_share
    return jnp.where(chosen, fast_rate, slow_rate).astype(jnp.float32)


def draw_extra_decay(key, part):
    level_key, rough_key, position_random_key, amount_random_key = jax.random.split(jax.random.fold_in(key, 23), 4)
    block_count = SEQUENCE_TOKENS // TOK_DEV
    levels = jnp.exp(jax.random.uniform(level_key, (block_count,), jnp.float32, math.log(0.15), math.log(0.6))) / SEQUENCE_TOKENS
    per_position = jnp.repeat(levels, TOK_DEV)
    rough = jax.random.uniform(rough_key, (SEQUENCE_TOKENS, RECURRENT_HEADS), jnp.float32, 0.5, 1.5)
    baseline_term = per_position[:, None] * rough
    spike_positions = jax.random.randint(position_random_key, (3,), 0, SEQUENCE_TOKENS)
    spike_magnitudes = jax.random.uniform(amount_random_key, (3, RECURRENT_HEADS), jnp.float32, 0.22, 0.51)
    spike_marks = (jnp.arange(SEQUENCE_TOKENS)[:, None] == spike_positions[None, :]).astype(jnp.float32)
    spike_values = jnp.dot(spike_marks, spike_magnitudes)
    return (baseline_term + spike_values).astype(jnp.float32)


def query_key_pair(key):
    query_seed, key_seed = jax.random.split(jax.random.fold_in(key, 37))
    spread = 1.3 / math.sqrt(D)
    query_weight = jnp.clip(jax.random.normal(query_seed, (D, DA_HEADS * 2 * HEAD), jnp.float32), -6.0, 6.0) * spread
    key_weight = jnp.clip(jax.random.normal(key_seed, (D, KV_HEADS * 2 * HEAD), jnp.float32), -6.0, 6.0) * spread
    return (query_weight, key_weight)


def draw_w_query(key, part):
    return query_key_pair(key)[0].astype(jnp.bfloat16)


def draw_w_key(key, part):
    return query_key_pair(key)[1].astype(jnp.bfloat16)


def block_scale(own_key, dims, shards, low, largest):
    def one(position, shards_of):
        draws = jax.random.uniform(jax.random.fold_in(jax.random.fold_in(own_key, 6), position), (shards_of,), jnp.float32, low / len(shards), largest / len(shards))
        return jnp.repeat(jnp.exp(draws), dims[position] // shards_of).reshape((-1,) + (1,) * (len(dims) - position - 1))

    factor_of = one(*shards[0])
    for cut in shards[1:]:
        factor_of = factor_of * one(*cut)
    return factor_of


def centred(own_key, dims, deviation, reach, shards=(), kind=jnp.bfloat16):
    gain = block_scale(own_key, dims, shards, -0.22, 0.18) if shards else 1.0
    values = jax.random.normal(own_key, dims, jnp.float32) * deviation * gain
    return jnp.minimum(jnp.maximum(values, -reach), reach).astype(kind)


def setup_inputs(seed: int = 0, part: int = 0) -> dict:
    key_of = jax.random.split(jax.random.key(seed), 17)
    own_keys = jax.random.split(jax.random.fold_in(key_of[16], part), 17)
    return {
        "tokens": centred(own_keys[0], (SEQUENCE_TOKENS, D), 1.0, 6.0, ((0, 4), (1, 2))),
        "norm_gain": jnp.clip(1.0 + 0.18 * jax.random.normal(key_of[1], (D,), jnp.float32), 0.1, 1.9),
        "w_recur_in": centred(key_of[2], (D, RG_W), D ** -0.5, 0.125, ((1, 2),)),
        "conv_weight": centred(key_of[3], (CONV, RG_W), CONV ** -0.5, 3.0, ((1, 2),), jnp.float32),
        "w_gate_decay": centred(key_of[4], (RECURRENT_HEADS, HEAD, HEAD), HEAD ** -0.5, 0.75, ((0, 2),)),
        "w_gate_input": centred(key_of[5], (RECURRENT_HEADS, HEAD, HEAD), HEAD ** -0.5, 0.75, ((0, 2),)),
        "decay_base": draw_decay_base(jax.random.fold_in(key_of[16], 71), part),
        "extra_decay": draw_extra_decay(jax.random.fold_in(jax.random.fold_in(key_of[16], part), 71), part),
        "w_query": draw_w_query(jax.random.fold_in(key_of[16], 71), part),
        "w_key": draw_w_key(jax.random.fold_in(key_of[16], 71), part),
        "w_value": centred(key_of[10], (D, KV_HEADS * DV), D ** -0.5, 0.125, ((1, 2),)),
        "mix_lambda": jnp.clip(0.3 + 0.5 * jax.random.uniform(key_of[11], (DA_HEADS,), jnp.float32) ** block_scale(key_of[11], (DA_HEADS,), ((0, 2),), -0.2, 0.2), 0.3, 0.8),
        "head_gain": jnp.clip(1.0 + 0.18 * jax.random.normal(key_of[12], (DV,), jnp.float32), 0.1, 1.9),
        "w_out_recur": centred(key_of[13], (RG_W, D), (RG_W + DA_HEADS * DV) ** -0.5, 0.125, ((0, 2),)),
        "w_out_attend": centred(key_of[14], (DA_HEADS * DV, D), (RG_W + DA_HEADS * DV) ** -0.5, 0.125, ((0, 2),)),
        "out_gain": jnp.clip(1.0 + 0.18 * jax.random.normal(key_of[15], (D,), jnp.float32), 0.1, 1.9),
    }


lru_rate = 8.0
norm_eps = 1e-06

def chain(earlier, later):
    return (earlier[0] * later[0], later[0] * earlier[1] + later[1])

def reference(tokens, norm_gain, w_recur_in, conv_weight, w_gate_decay, w_gate_input, decay_base, extra_decay, w_query, w_key, w_value, mix_lambda, head_gain, w_out_recur, w_out_attend, out_gain):
    flat = tokens.astype(jnp.float32)
    inverse = lax.rsqrt(lax.optimization_barrier(jnp.mean(flat * flat, axis=1, keepdims=True)) + norm_eps)
    scaled = (flat * norm_gain).astype(jnp.bfloat16)

    def project(weight):
        return (jnp.dot(scaled, weight, preferred_element_type=jnp.float32) * inverse).astype(jnp.bfloat16)
    recur_in = project(w_recur_in)
    queries = project(w_query)
    keys = project(w_key)
    values = project(w_value)
    padded = jnp.concatenate([jnp.zeros((CONV - 1, RG_W), jnp.bfloat16), recur_in], axis=0).astype(jnp.float32)
    conv_acc = jnp.zeros((SEQUENCE_TOKENS, RG_W), jnp.float32)
    for offset in range(CONV):
        conv_acc = conv_acc + conv_weight[offset] * padded[offset:offset + SEQUENCE_TOKENS]
    conv_in = conv_acc.astype(jnp.bfloat16)
    blocks = conv_in.astype(jnp.float32).reshape(SEQUENCE_TOKENS, RECURRENT_HEADS, HEAD)
    decay_gate = jax.nn.sigmoid(jnp.einsum('thi,hij->thj', blocks, w_gate_decay.astype(jnp.float32))).reshape(SEQUENCE_TOKENS, RG_W)
    input_gate = jax.nn.sigmoid(jnp.einsum('thi,hij->thj', blocks, w_gate_input.astype(jnp.float32))).reshape(SEQUENCE_TOKENS, RG_W)
    log_decay = -lru_rate * decay_gate * decay_base - jnp.repeat(extra_decay, HEAD, axis=1)
    decay = jnp.exp(log_decay)
    inject = jnp.sqrt(-jnp.expm1(2.0 * log_decay)) * input_gate * conv_in.astype(jnp.float32)
    unused_total, states = lax.associative_scan(chain, (decay, inject), axis=0)
    recur_out = states.astype(jnp.bfloat16)
    group_size = DA_HEADS // KV_HEADS
    query_four = queries.reshape(SEQUENCE_TOKENS, KV_HEADS, group_size, 2, HEAD)
    key_three = keys.reshape(SEQUENCE_TOKENS, KV_HEADS, 2, HEAD).astype(jnp.float32)
    value_three = values.reshape(SEQUENCE_TOKENS, KV_HEADS, DV).astype(jnp.float32)
    block_rows = math.gcd(SEQUENCE_TOKENS, 512)
    positions = jnp.arange(SEQUENCE_TOKENS, dtype=jnp.int32)
    lambdas = mix_lambda.reshape(KV_HEADS, group_size)

    def one_block(index):
        begin = (index * block_rows).astype(jnp.int32)
        query_part = lax.dynamic_slice_in_dim(query_four, begin, block_rows, 0).astype(jnp.float32)
        allowed = (begin + jnp.arange(block_rows, dtype=jnp.int32))[:, None] >= positions[None, :]
        results = []
        for mapping in range(2):
            scores = jnp.einsum('bkgd,tkd->kgbt', query_part[:, :, :, mapping, :], key_three[:, :, mapping, :]) * HEAD ** (-0.5)
            scores = jnp.where(allowed, scores, -jnp.inf)
            peak = lax.optimization_barrier(jnp.max(scores, axis=-1, keepdims=True))
            expo = jnp.exp(scores - peak)
            total = lax.optimization_barrier(jnp.sum(expo, axis=-1))
            rounded = lax.optimization_barrier(expo.astype(jnp.bfloat16)).astype(jnp.float32)
            attend = jnp.einsum('kgbt,tke->bkge', rounded, value_three)
            results.append(attend / jnp.transpose(total, (2, 0, 1))[..., None])
        return results[0] - lambdas[None, :, :, None] * results[1]
    head_out = lax.map(one_block, jnp.arange(SEQUENCE_TOKENS // block_rows, dtype=jnp.int32))
    head_out = head_out.reshape(SEQUENCE_TOKENS, DA_HEADS, DV)
    normed = head_out * lax.rsqrt(lax.optimization_barrier(jnp.mean(head_out * head_out, axis=-1, keepdims=True)) + norm_eps) * head_gain
    attend_out = normed.astype(jnp.bfloat16).reshape(SEQUENCE_TOKENS, DA_HEADS * DV)
    merged = jnp.dot(recur_out, w_out_recur, preferred_element_type=jnp.float32) + jnp.dot(attend_out, w_out_attend, preferred_element_type=jnp.float32)
    final = merged * lax.rsqrt(lax.optimization_barrier(jnp.mean(merged * merged, axis=1, keepdims=True)) + norm_eps) * out_gain
    return final.astype(jnp.bfloat16)
```

```python
import functools

import jax
import jax.numpy as jnp
from jax import lax
from jax.experimental import pallas as pl
from jax.experimental.pallas import tpu as pltpu
from jax.sharding import PartitionSpec as P

HEAD = 64
PAIR = 2 * HEAD
MESH = pl.DeviceIdType.MESH
F32 = jnp.float32
BF16 = jnp.bfloat16

lru_rate = 8.0
norm_eps = 1e-06


def dot(a, b):
    return jnp.dot(a, b, preferred_element_type=F32)


def minus_expm1(y):
    series = 1.0 + y * (1.0 / 6.0)
    for k in (5.0, 4.0, 3.0, 2.0):
        series = 1.0 + y * (1.0 / k) * series
    return jnp.where(y > -0.25, -y * series, 1.0 - jnp.exp(y))


def kernel(
    sp_size,
    tp_size,
    taps,
    tokens,
    norm_gain,
    w_recur_in,
    conv_weight,
    w_gate_decay,
    w_gate_input,
    decay_base,
    extra_decay,
    w_query,
    w_key,
    w_value,
    mix_lambda,
    head_gain,
    w_out_recur,
    w_out_attend,
    out_gain,
    out,
    tok,
    scaled,
    wkv,
    wr,
    wq,
    wor,
    woa,
    v_norm_gain,
    v_conv,
    v_gate_decay,
    v_gate_input,
    v_base,
    v_extra,
    v_head_gain,
    v_out_gain,
    gates,
    acc_kv,
    acc_r,
    acc_q,
    kv,
    rbuf,
    qbuf,
    peaks,
    totals,
    attends,
    cum_decay,
    local_state,
    carry_out,
    carry_in,
    carried,
    attend_out,
    merged,
    part_out,
    part_in,
    load_sem,
    tok_sem,
    kv_send,
    kv_recv,
    halo_sem,
    carry_send,
    carry_recv,
    part_send,
    part_recv,
):
    me = lax.axis_index("sp")
    core = lax.axis_index("tp")
    partner = 1 - core
    rows, half = tokens.shape
    width = half * tp_size
    recur_cols = wr.shape[1]
    key_cols = w_key.shape[1]
    query_cols = wq.shape[1]
    kv_local = key_cols // PAIR
    heads = query_cols // PAIR
    group = heads // kv_local
    halo = rbuf.shape[0] - rows
    own_rows = rows // tp_size
    chunks, _, chunk = part_out.shape

    barrier = pltpu.get_barrier_semaphore()
    pl.semaphore_signal(barrier, inc=1, device_id={"tp": partner}, device_id_type=MESH)
    for step in range(1, sp_size):
        other = lax.rem(me + step, sp_size)
        pl.semaphore_signal(barrier, inc=1, device_id={"sp": other}, device_id_type=MESH)

    mine = pl.ds(pl.multiple_of(core * half, half), half)
    theirs = pl.ds(pl.multiple_of(partner * half, half), half)
    plan = {}

    def load(name, src, dst):
        copy = pltpu.make_async_copy(src, dst, load_sem.at[len(plan)])
        copy.start()
        plan[name] = copy

    load("tok", tokens, tok.at[core])
    load("norm_gain", norm_gain, v_norm_gain)
    load("k0", w_key.at[mine], wkv.at[mine, pl.ds(0, key_cols)])
    load("v0", w_value.at[mine], wkv.at[mine, pl.ds(key_cols, wkv.shape[1] - key_cols)])
    load("r0", w_recur_in.at[mine], wr.at[mine])
    load("q0", w_query.at[mine], wq.at[mine])
    load("k1", w_key.at[theirs], wkv.at[theirs, pl.ds(0, key_cols)])
    load("v1", w_value.at[theirs], wkv.at[theirs, pl.ds(key_cols, wkv.shape[1] - key_cols)])
    load("r1", w_recur_in.at[theirs], wr.at[theirs])
    load("q1", w_query.at[theirs], wq.at[theirs])
    load("gate_decay", w_gate_decay, v_gate_decay)
    load("gate_input", w_gate_input, v_gate_input)
    load("conv", conv_weight, v_conv)
    load("base", decay_base, v_base)
    load("extra", extra_decay, v_extra)
    load("head_gain", head_gain, v_head_gain)
    load("out_gain", out_gain, v_out_gain)
    load("wor", w_out_recur, wor)
    load("woa", w_out_attend, woa)

    pl.semaphore_wait(barrier, sp_size)
    tok_copy = pltpu.make_async_remote_copy(
        tokens, tok.at[core], tok_sem.at[0], tok_sem.at[1],
        device_id={"tp": partner}, device_id_type=MESH,
    )
    tok_copy.start()

    def scale(part, columns):
        wide = tok[part].astype(F32)
        scaled[part] = (wide * v_norm_gain[:, columns]).astype(BF16)
        return jnp.sum(wide * wide, axis=1, keepdims=True)

    plan["tok"].wait()
    plan["norm_gain"].wait()
    squares = scale(core, mine)
    own = scaled[core]
    plan["k0"].wait()
    plan["v0"].wait()
    acc_kv[...] = dot(own, wkv[mine, :])
    plan["r0"].wait()
    acc_r[...] = dot(own, wr[mine, :])
    plan["q0"].wait()
    acc_q[...] = dot(own, wq[mine, :])

    tok_copy.wait_recv()
    squares = squares + scale(partner, theirs)
    inverse = lax.rsqrt(squares / width + norm_eps)
    far = scaled[partner]
    plan["k1"].wait()
    plan["v1"].wait()
    kv[me] = ((acc_kv[...] + dot(far, wkv[theirs, :])) * inverse).astype(BF16)

    def kv_copy(step):
        return pltpu.make_async_remote_copy(
            kv.at[me], kv.at[me], kv_send.at[step], kv_recv.at[step],
            device_id={"sp": lax.rem(me + step, sp_size)}, device_id_type=MESH,
        )

    def kv_arrival(step):
        slot = kv.at[me - step]
        return pltpu.make_async_remote_copy(
            slot, slot, kv_send.at[step], kv_recv.at[step],
            device_id={"sp": lax.rem(me + step, sp_size)}, device_id_type=MESH,
        )

    for step in range(1, sp_size):
        @pl.when(me + step < sp_size)
        def _():
            kv_copy(step).start()

    plan["r1"].wait()
    rbuf[pl.ds(halo, rows), :] = ((acc_r[...] + dot(far, wr[theirs, :])) * inverse).astype(BF16)
    halo_copy = pltpu.make_async_remote_copy(
        rbuf.at[pl.ds(rows, halo)], rbuf.at[pl.ds(0, halo)], halo_sem.at[0], halo_sem.at[1],
        device_id={"sp": lax.rem(me + 1, sp_size)}, device_id_type=MESH,
    )

    @pl.when(me + 1 < sp_size)
    def _():
        halo_copy.start()

    @pl.when(me == 0)
    def _():
        rbuf[pl.ds(0, halo), :] = jnp.zeros((halo, recur_cols), BF16)

    plan["q1"].wait()
    query = (acc_q[...] + dot(far, wq[theirs, :])) * (inverse * HEAD ** (-0.5))
    for h in range(heads):
        qbuf[h] = query[:, h * PAIR : (h + 1) * PAIR].astype(BF16)

    lane = lax.broadcasted_iota(jnp.int32, (rows, PAIR), 1)
    row = lax.broadcasted_iota(jnp.int32, (rows, PAIR), 0)
    low = lane < HEAD

    def attend(block, first):
        for g in range(kv_local):
            keys = kv[block, :, g * PAIR : (g + 1) * PAIR].astype(F32)
            value = kv[block, :, key_cols + g * PAIR : key_cols + (g + 1) * PAIR]
            both = jnp.concatenate(
                [jnp.where(low, keys, 0.0).astype(BF16), jnp.where(low, 0.0, keys).astype(BF16)], 0
            )
            for h in range(g * group, (g + 1) * group):
                scores = lax.dot_general(
                    qbuf[h], both, (((1,), (1,)), ((), ())), preferred_element_type=F32
                )
                for m in range(2):
                    score = scores[:, m * rows : (m + 1) * rows]
                    if first:
                        score = jnp.where(row >= lane, score, -jnp.inf)
                    top = jnp.broadcast_to(jnp.max(score, axis=1, keepdims=True), score.shape)
                    if first:
                        peak = top
                        expo = jnp.exp(score - peak)
                        totals[h, m] = expo
                        attends[h, m] = dot(expo.astype(BF16), value)
                    else:
                        before = peaks[h, m]
                        peak = jnp.maximum(before, top)
                        fix = jnp.exp(before - peak)
                        expo = jnp.exp(score - peak)
                        totals[h, m] = totals[h, m] * fix + expo
                        attends[h, m] = attends[h, m] * fix + dot(expo.astype(BF16), value)
                    peaks[h, m] = peak

    attend(me, True)

    plan["gate_decay"].wait()
    plan["gate_input"].wait()
    blank = jnp.zeros((HEAD, HEAD), F32)
    pairs = gates.shape[0]
    for p in range(pairs):
        for column, source in enumerate((v_gate_decay, v_gate_input)):
            upper = jnp.concatenate([source[2 * p].astype(F32), blank], 1)
            lower = jnp.concatenate([blank, source[2 * p + 1].astype(F32)], 1)
            gates[p, :, column * PAIR : (column + 1) * PAIR] = jnp.concatenate(
                [upper, lower], 0
            ).astype(BF16)

    for name in ("conv", "base", "extra"):
        plan[name].wait()

    @pl.when(me > 0)
    def _():
        halo_copy.wait_recv()

    start = halo - (taps - 1)
    for p in range(pairs):
        columns = slice(p * PAIR, (p + 1) * PAIR)
        padded = rbuf[:, columns].astype(F32)
        conv = jnp.zeros((rows, PAIR), F32)
        for k in range(taps):
            conv = conv + v_conv[k : k + 1, columns] * padded[start + k : start + k + rows]
        conv_in = conv.astype(BF16)
        logits = dot(conv_in, gates[p])
        decay_gate = jax.nn.sigmoid(logits[:, :PAIR])
        input_gate = jax.nn.sigmoid(logits[:, PAIR:])
        extra = jnp.where(
            low,
            jnp.broadcast_to(v_extra[:, 2 * p : 2 * p + 1], (rows, PAIR)),
            jnp.broadcast_to(v_extra[:, 2 * p + 1 : 2 * p + 2], (rows, PAIR)),
        )
        log_decay = -lru_rate * decay_gate * v_base[:, columns] - extra
        decay = jnp.exp(log_decay)
        state = jnp.sqrt(minus_expm1(2.0 * log_decay)) * input_gate * conv_in.astype(F32)
        reach = 1
        while reach < rows:
            if reach < 8:
                earlier = row >= reach
                decay_before = jnp.where(earlier, pltpu.roll(decay, reach, 0), 1.0)
                state_before = jnp.where(earlier, pltpu.roll(state, reach, 0), 0.0)
            else:
                decay_before = jnp.concatenate(
                    [jnp.ones((reach, PAIR), F32), decay[: rows - reach]], 0
                )
                state_before = jnp.concatenate(
                    [jnp.zeros((reach, PAIR), F32), state[: rows - reach]], 0
                )
            state = decay * state_before + state
            decay = decay * decay_before
            reach *= 2
        cum_decay[:, columns] = decay
        local_state[:, columns] = state
        carry_out[0:1, columns] = decay[rows - 1 :]
        carry_out[1:2, columns] = state[rows - 1 :]

    def carry_copy(step, slot):
        return pltpu.make_async_remote_copy(
            carry_out, carry_in.at[slot], carry_send.at[step], carry_recv.at[step],
            device_id={"sp": lax.rem(me + step, sp_size)}, device_id_type=MESH,
        )

    for step in range(1, sp_size):
        @pl.when(me + step < sp_size)
        def _():
            carry_copy(step, me).start()

    def one(step, unused):
        kv_arrival(step).wait_recv()
        attend(me - step, False)
        return unused

    lax.fori_loop(1, me, one, 0)

    carried[...] = jnp.zeros_like(carried)

    def link(back, unused):
        step = me - back
        carry_copy(step, back).wait_recv()
        carried[...] = carry_in[back, 0:1] * carried[...] + carry_in[back, 1:2]
        return unused

    lax.fori_loop(0, me, link, 0)
    recur_out = (local_state[...] + cum_decay[...] * carried[...]).astype(BF16)
    plan["wor"].wait()
    for c in range(chunks):
        columns = slice(c * chunk, (c + 1) * chunk)
        merged[:, columns] = dot(recur_out, wor[:, columns])

    lax.fori_loop(jnp.maximum(me, 1), me + 1, one, 0)

    plan["head_gain"].wait()
    for h in range(heads):
        first, second = (
            attends[h, m] / jnp.sum(totals[h, m], axis=1, keepdims=True) for m in range(2)
        )
        head_out = first - mix_lambda[0, h] * second
        normed = (
            head_out
            * lax.rsqrt(jnp.mean(head_out * head_out, axis=1, keepdims=True) + norm_eps)
            * v_head_gain[...]
        )
        attend_out[:, h * PAIR : (h + 1) * PAIR] = normed.astype(BF16)

    plan["woa"].wait()
    attended = attend_out[...]

    def part_copy(c):
        return pltpu.make_async_remote_copy(
            part_out.at[c], part_in.at[c], part_send.at[c], part_recv.at[c],
            device_id={"tp": partner}, device_id_type=MESH,
        )

    keep = pl.ds(pl.multiple_of(core * own_rows, own_rows), own_rows)
    give = pl.ds(pl.multiple_of(partner * own_rows, own_rows), own_rows)
    for c in range(chunks):
        columns = slice(c * chunk, (c + 1) * chunk)
        merged[:, columns] = merged[:, columns] + dot(attended, woa[:, columns])
        part_out[c] = merged[give, columns].astype(BF16)
        part_copy(c).start()

    plan["out_gain"].wait()
    squares = jnp.zeros((own_rows, 1), F32)
    for c in range(chunks):
        columns = slice(c * chunk, (c + 1) * chunk)
        part_copy(c).wait_recv()
        whole = merged[keep, columns] + part_in[c].astype(F32)
        merged[keep, columns] = whole
        squares = squares + jnp.sum(whole * whole, axis=1, keepdims=True)
    final = lax.rsqrt(squares / out.shape[1] + norm_eps)
    for c in range(chunks):
        columns = slice(c * chunk, (c + 1) * chunk)
        out[:, columns] = (merged[keep, columns] * final * v_out_gain[:, columns]).astype(BF16)

    tok_copy.wait_send()
    for c in range(chunks):
        part_copy(c).wait_send()

    @pl.when(me + 1 < sp_size)
    def _():
        halo_copy.wait_send()

    for step in range(1, sp_size):
        @pl.when(me + step < sp_size)
        def _():
            kv_copy(step).wait_send()
            carry_copy(step, me).wait_send()


def body(sp_size, tp_size, *args):
    (tokens, norm_gain, w_recur_in, conv_weight, w_gate_decay, w_gate_input, decay_base,
     extra_decay, w_query, w_key, w_value, mix_lambda, head_gain, w_out_recur, w_out_attend,
     out_gain) = args
    rows, half = tokens.shape
    width = w_recur_in.shape[0]
    recur_cols, query_cols = w_recur_in.shape[1], w_query.shape[1]
    kv_cols = w_key.shape[1] + w_value.shape[1]
    heads = query_cols // PAIR
    pairs = recur_cols // PAIR
    out_width = w_out_recur.shape[1]
    chunk = min(512, out_width)
    chunks = out_width // chunk
    own_rows = rows // tp_size
    halo = 16
    line = lambda a: a.reshape(1, -1)
    operands = (tokens, line(norm_gain), w_recur_in, conv_weight, w_gate_decay, w_gate_input,
                line(decay_base), extra_decay, w_query, w_key, w_value, line(mix_lambda),
                line(head_gain), w_out_recur, w_out_attend, line(out_gain))
    anywhere = pl.BlockSpec(memory_space=pl.ANY)
    specs = [anywhere] * len(operands)
    specs[11] = pl.BlockSpec(memory_space=pltpu.SMEM)
    like = lambda a: pltpu.VMEM(a.shape, a.dtype)
    dma = lambda n: pltpu.SemaphoreType.DMA((n,))
    return pl.pallas_call(
        functools.partial(kernel, sp_size, tp_size, conv_weight.shape[0]),
        out_shape=jax.ShapeDtypeStruct((own_rows, out_width), BF16),
        in_specs=specs,
        out_specs=pl.BlockSpec(memory_space=pltpu.VMEM),
        scratch_shapes=[
            pltpu.VMEM((tp_size, rows, half), BF16),
            pltpu.VMEM((tp_size, rows, half), BF16),
            pltpu.VMEM((width, kv_cols), BF16),
            like(w_recur_in),
            like(w_query),
            like(w_out_recur),
            like(w_out_attend),
            like(operands[1]),
            like(conv_weight),
            like(w_gate_decay),
            like(w_gate_input),
            like(operands[6]),
            like(extra_decay),
            like(operands[12]),
            like(operands[15]),
            pltpu.VMEM((pairs, PAIR, 2 * PAIR), BF16),
            pltpu.VMEM((rows, kv_cols), F32),
            pltpu.VMEM((rows, recur_cols), F32),
            pltpu.VMEM((rows, query_cols), F32),
            pltpu.VMEM((sp_size, rows, kv_cols), BF16),
            pltpu.VMEM((halo + rows, recur_cols), BF16),
            pltpu.VMEM((heads, rows, PAIR), BF16),
            pltpu.VMEM((heads, 2, rows, PAIR), F32),
            pltpu.VMEM((heads, 2, rows, PAIR), F32),
            pltpu.VMEM((heads, 2, rows, PAIR), F32),
            pltpu.VMEM((rows, recur_cols), F32),
            pltpu.VMEM((rows, recur_cols), F32),
            pltpu.VMEM((2, recur_cols), F32),
            pltpu.VMEM((sp_size, 2, recur_cols), F32),
            pltpu.VMEM((1, recur_cols), F32),
            pltpu.VMEM((rows, query_cols), BF16),
            pltpu.VMEM((rows, out_width), F32),
            pltpu.VMEM((chunks, own_rows, chunk), BF16),
            pltpu.VMEM((chunks, own_rows, chunk), BF16),
            dma(19),
            dma(2),
            dma(sp_size),
            dma(sp_size),
            dma(2),
            dma(sp_size),
            dma(sp_size),
            dma(chunks),
            dma(chunks),
        ],
        compiler_params=pltpu.CompilerParams(collective_id=0, has_side_effects=True),
        name="layer",
    )(*operands)


def solution(mesh):
    in_specs = (
        P(("fs", "sp"), "tp"),
        P(),
        P(None, "tp"),
        P(None, "tp"),
        P("tp", None, None),
        P("tp", None, None),
        P("tp"),
        P(("fs", "sp"), "tp"),
        P(None, "tp"),
        P(None, "tp"),
        P(None, "tp"),
        P("tp"),
        P(),
        P("tp", None),
        P("tp", None),
        P(),
    )
    out_specs = P(("fs", "sp", "tp"), None)
    return jax.shard_map(
        functools.partial(body, mesh.shape["sp"], mesh.shape["tp"]),
        mesh=mesh, in_specs=in_specs, out_specs=out_specs, check_vma=False,
    )
```

```python
import functools

import jax
import jax.numpy as jnp
from jax import lax
from jax.experimental import pallas as pl
from jax.experimental.pallas import tpu as pltpu
from jax.sharding import PartitionSpec as P

HEAD = 64
PAIR = 2 * HEAD
MESH = pl.DeviceIdType.MESH
F32 = jnp.float32
BF16 = jnp.bfloat16

lru_rate = 8.0
norm_eps = 1e-06


def dot(a, b):
    return jnp.dot(a, b, preferred_element_type=F32)


def minus_expm1(y):
    series = 1.0 + y * (1.0 / 6.0)
    for k in (5.0, 4.0, 3.0, 2.0):
        series = 1.0 + y * (1.0 / k) * series
    return jnp.where(y > -0.25, -y * series, 1.0 - jnp.exp(y))


def kernel(
    sp_size,
    tp_size,
    taps,
    tokens,
    norm_gain,
    w_recur_in,
    conv_weight,
    w_gate_decay,
    w_gate_input,
    decay_base,
    extra_decay,
    w_query,
    w_key,
    w_value,
    mix_lambda,
    head_gain,
    w_out_recur,
    w_out_attend,
    out_gain,
    out,
    tok,
    scaled,
    wkv,
    wr,
    wq,
    wor,
    woa,
    v_norm_gain,
    v_conv,
    v_gate_decay,
    v_gate_input,
    v_base,
    v_extra,
    v_head_gain,
    v_out_gain,
    gates,
    acc_kv,
    acc_r,
    acc_q,
    kv,
    rbuf,
    qbuf,
    peaks,
    totals,
    attends,
    cum_decay,
    local_state,
    carry_out,
    carry_in,
    carried,
    attend_out,
    merged,
    part_out,
    part_in,
    load_sem,
    tok_sem,
    kv_send,
    kv_recv,
    halo_sem,
    carry_send,
    carry_recv,
    part_send,
    part_recv,
):
    me = lax.axis_index("sp")
    core = lax.axis_index("tp")
    partner = 1 - core
    rows, half = tokens.shape
    width = half * tp_size
    recur_cols = wr.shape[1]
    key_cols = w_key.shape[1]
    query_cols = wq.shape[1]
    kv_local = key_cols // PAIR
    heads = query_cols // PAIR
    group = heads // kv_local
    halo = rbuf.shape[0] - rows
    own_rows = rows // tp_size
    chunks, _, chunk = part_out.shape

    barrier = pltpu.get_barrier_semaphore()
    pl.semaphore_signal(barrier, inc=1, device_id={"tp": partner}, device_id_type=MESH)
    for step in range(1, sp_size):
        other = lax.rem(me + step, sp_size)
        pl.semaphore_signal(barrier, inc=1, device_id={"sp": other}, device_id_type=MESH)

    mine = pl.ds(pl.multiple_of(core * half, half), half)
    theirs = pl.ds(pl.multiple_of(partner * half, half), half)
    plan = {}

    def load(name, src, dst):
        copy = pltpu.make_async_copy(src, dst, load_sem.at[len(plan)])
        copy.start()
        plan[name] = copy

    load("tok", tokens, tok.at[core])
    load("norm_gain", norm_gain, v_norm_gain)
    load("r0", w_recur_in.at[mine], wr.at[mine])
    load("k0", w_key.at[mine], wkv.at[mine, pl.ds(0, key_cols)])
    load("v0", w_value.at[mine], wkv.at[mine, pl.ds(key_cols, wkv.shape[1] - key_cols)])
    load("r1", w_recur_in.at[theirs], wr.at[theirs])
    load("k1", w_key.at[theirs], wkv.at[theirs, pl.ds(0, key_cols)])
    load("v1", w_value.at[theirs], wkv.at[theirs, pl.ds(key_cols, wkv.shape[1] - key_cols)])

    pl.semaphore_wait(barrier, sp_size)
    plan["tok"].wait()
    tok_copy = pltpu.make_async_remote_copy(
        tok.at[core], tok.at[core], tok_sem.at[0], tok_sem.at[1],
        device_id={"tp": partner}, device_id_type=MESH,
    )
    tok_copy.start()

    def scale(part, columns):
        wide = tok[part].astype(F32)
        scaled[part] = (wide * v_norm_gain[:, columns]).astype(BF16)
        return jnp.sum(wide * wide, axis=1, keepdims=True)

    load("q0", w_query.at[mine], wq.at[mine])
    load("q1", w_query.at[theirs], wq.at[theirs])
    plan["norm_gain"].wait()
    squares = scale(core, mine)
    own = scaled[core]
    plan["r0"].wait()
    acc_r[...] = dot(own, wr[mine, :])
    plan["k0"].wait()
    plan["v0"].wait()
    acc_kv[...] = dot(own, wkv[mine, :])
    plan["q0"].wait()
    acc_q[...] = dot(own, wq[mine, :])

    load("gate_decay", w_gate_decay, v_gate_decay)
    load("gate_input", w_gate_input, v_gate_input)
    load("conv", conv_weight, v_conv)
    load("base", decay_base, v_base)
    load("extra", extra_decay, v_extra)
    load("head_gain", head_gain, v_head_gain)
    load("out_gain", out_gain, v_out_gain)
    load("wor", w_out_recur, wor)
    load("woa", w_out_attend, woa)
    tok_copy.wait_recv()
    squares = squares + scale(partner, theirs)
    inverse = lax.rsqrt(squares / width + norm_eps)
    far = scaled[partner]
    plan["r1"].wait()
    rbuf[pl.ds(halo, rows), :] = ((acc_r[...] + dot(far, wr[theirs, :])) * inverse).astype(BF16)
    halo_copy = pltpu.make_async_remote_copy(
        rbuf.at[pl.ds(rows, halo)], rbuf.at[pl.ds(0, halo)], halo_sem.at[0], halo_sem.at[1],
        device_id={"sp": lax.rem(me + 1, sp_size)}, device_id_type=MESH,
    )

    @pl.when(me + 1 < sp_size)
    def _():
        halo_copy.start()

    @pl.when(me == 0)
    def _():
        rbuf[pl.ds(0, halo), :] = jnp.zeros((halo, recur_cols), BF16)

    plan["k1"].wait()
    plan["v1"].wait()
    kv[me] = ((acc_kv[...] + dot(far, wkv[theirs, :])) * inverse).astype(BF16)

    def kv_copy(step):
        return pltpu.make_async_remote_copy(
            kv.at[me], kv.at[me], kv_send.at[step], kv_recv.at[step],
            device_id={"sp": lax.rem(me + step, sp_size)}, device_id_type=MESH,
        )

    def kv_arrival(step):
        slot = kv.at[me - step]
        return pltpu.make_async_remote_copy(
            slot, slot, kv_send.at[step], kv_recv.at[step],
            device_id={"sp": lax.rem(me + step, sp_size)}, device_id_type=MESH,
        )

    for step in range(1, sp_size):
        @pl.when(me + step < sp_size)
        def _():
            kv_copy(step).start()

    plan["q1"].wait()
    query = (acc_q[...] + dot(far, wq[theirs, :])) * (inverse * HEAD ** (-0.5))
    for h in range(heads):
        qbuf[h] = query[:, h * PAIR : (h + 1) * PAIR].astype(BF16)

    lane = lax.broadcasted_iota(jnp.int32, (rows, PAIR), 1)
    row = lax.broadcasted_iota(jnp.int32, (rows, PAIR), 0)
    low = lane < HEAD

    def attend(block, first):
        for g in range(kv_local):
            keys = kv[block, :, g * PAIR : (g + 1) * PAIR].astype(F32)
            value = kv[block, :, key_cols + g * PAIR : key_cols + (g + 1) * PAIR]
            both = jnp.concatenate(
                [jnp.where(low, keys, 0.0).astype(BF16), jnp.where(low, 0.0, keys).astype(BF16)], 0
            )
            for h in range(g * group, (g + 1) * group):
                scores = lax.dot_general(
                    qbuf[h], both, (((1,), (1,)), ((), ())), preferred_element_type=F32
                )
                for m in range(2):
                    score = scores[:, m * rows : (m + 1) * rows]
                    if first:
                        score = jnp.where(row >= lane, score, -jnp.inf)
                    top = jnp.broadcast_to(jnp.max(score, axis=1, keepdims=True), score.shape)
                    if first:
                        peak = top
                        expo = jnp.exp(score - peak)
                        totals[h, m] = expo
                        attends[h, m] = dot(expo.astype(BF16), value)
                    else:
                        before = peaks[h, m]
                        peak = jnp.maximum(before, top)
                        fix = jnp.exp(before - peak)
                        expo = jnp.exp(score - peak)
                        totals[h, m] = totals[h, m] * fix + expo
                        attends[h, m] = attends[h, m] * fix + dot(expo.astype(BF16), value)
                    peaks[h, m] = peak

    attend(me, True)

    plan["gate_decay"].wait()
    plan["gate_input"].wait()
    blank = jnp.zeros((HEAD, HEAD), F32)
    pairs = gates.shape[0]
    for p in range(pairs):
        for column, source in enumerate((v_gate_decay, v_gate_input)):
            upper = jnp.concatenate([source[2 * p].astype(F32), blank], 1)
            lower = jnp.concatenate([blank, source[2 * p + 1].astype(F32)], 1)
            gates[p, :, column * PAIR : (column + 1) * PAIR] = jnp.concatenate(
                [upper, lower], 0
            ).astype(BF16)

    for name in ("conv", "base", "extra"):
        plan[name].wait()

    @pl.when(me > 0)
    def _():
        halo_copy.wait_recv()

    start = halo - (taps - 1)
    spread = v_extra[...].T
    for p in range(pairs):
        columns = slice(p * PAIR, (p + 1) * PAIR)
        padded = rbuf[:, columns].astype(F32)
        conv = jnp.zeros((rows, PAIR), F32)
        for k in range(taps):
            conv = conv + v_conv[k : k + 1, columns] * padded[start + k : start + k + rows]
        conv_in = conv.astype(BF16)
        logits = dot(conv_in, gates[p])
        decay_gate = jax.nn.sigmoid(logits[:, :PAIR])
        input_gate = jax.nn.sigmoid(logits[:, PAIR:])
        extra = jnp.where(
            low,
            jnp.broadcast_to(spread[:, 2 * p : 2 * p + 1], (rows, PAIR)),
            jnp.broadcast_to(spread[:, 2 * p + 1 : 2 * p + 2], (rows, PAIR)),
        )
        log_decay = -lru_rate * decay_gate * v_base[:, columns] - extra
        decay = jnp.exp(log_decay)
        state = jnp.sqrt(minus_expm1(2.0 * log_decay)) * input_gate * conv_in.astype(F32)
        reach = 1
        while reach < rows:
            if reach < 8:
                earlier = row >= reach
                decay_before = jnp.where(earlier, pltpu.roll(decay, reach, 0), 1.0)
                state_before = jnp.where(earlier, pltpu.roll(state, reach, 0), 0.0)
            else:
                decay_before = jnp.concatenate(
                    [jnp.ones((reach, PAIR), F32), decay[: rows - reach]], 0
                )
                state_before = jnp.concatenate(
                    [jnp.zeros((reach, PAIR), F32), state[: rows - reach]], 0
                )
            state = decay * state_before + state
            decay = decay * decay_before
            reach *= 2
        cum_decay[:, columns] = decay
        local_state[:, columns] = state
        carry_out[0:1, columns] = decay[rows - 1 :]
        carry_out[1:2, columns] = state[rows - 1 :]

    def carry_copy(step, slot):
        return pltpu.make_async_remote_copy(
            carry_out, carry_in.at[slot], carry_send.at[step], carry_recv.at[step],
            device_id={"sp": lax.rem(me + step, sp_size)}, device_id_type=MESH,
        )

    for step in range(1, sp_size):
        @pl.when(me + step < sp_size)
        def _():
            carry_copy(step, me).start()

    def one(step, unused):
        kv_arrival(step).wait_recv()
        attend(me - step, False)
        return unused

    lax.fori_loop(1, me, one, 0)

    carried[...] = jnp.zeros_like(carried)

    def link(back, unused):
        step = me - back
        carry_copy(step, back).wait_recv()
        carried[...] = carry_in[back, 0:1] * carried[...] + carry_in[back, 1:2]
        return unused

    lax.fori_loop(0, me, link, 0)
    recur_out = (local_state[...] + cum_decay[...] * carried[...]).astype(BF16)
    plan["wor"].wait()
    for c in range(chunks):
        columns = slice(c * chunk, (c + 1) * chunk)
        merged[:, columns] = dot(recur_out, wor[:, columns])

    lax.fori_loop(jnp.maximum(me, 1), me + 1, one, 0)

    plan["head_gain"].wait()
    for h in range(heads):
        first, second = (
            attends[h, m] / jnp.sum(totals[h, m], axis=1, keepdims=True) for m in range(2)
        )
        head_out = first - mix_lambda[0, h] * second
        normed = (
            head_out
            * lax.rsqrt(jnp.mean(head_out * head_out, axis=1, keepdims=True) + norm_eps)
            * v_head_gain[...]
        )
        attend_out[:, h * PAIR : (h + 1) * PAIR] = normed.astype(BF16)

    plan["woa"].wait()
    attended = attend_out[...]

    def part_copy(c):
        return pltpu.make_async_remote_copy(
            part_out.at[c], part_in.at[c], part_send.at[c], part_recv.at[c],
            device_id={"tp": partner}, device_id_type=MESH,
        )

    keep = pl.ds(pl.multiple_of(core * own_rows, own_rows), own_rows)
    give = pl.ds(pl.multiple_of(partner * own_rows, own_rows), own_rows)
    for c in range(chunks):
        columns = slice(c * chunk, (c + 1) * chunk)
        merged[:, columns] = merged[:, columns] + dot(attended, woa[:, columns])
        part_out[c] = merged[give, columns].astype(BF16)
        part_copy(c).start()

    plan["out_gain"].wait()
    squares = jnp.zeros((own_rows, 1), F32)
    for c in range(chunks):
        columns = slice(c * chunk, (c + 1) * chunk)
        part_copy(c).wait_recv()
        whole = merged[keep, columns] + part_in[c].astype(F32)
        merged[keep, columns] = whole
        squares = squares + jnp.sum(whole * whole, axis=1, keepdims=True)
    final = lax.rsqrt(squares / out.shape[1] + norm_eps)
    for c in range(chunks):
        columns = slice(c * chunk, (c + 1) * chunk)
        out[:, columns] = (merged[keep, columns] * final * v_out_gain[:, columns]).astype(BF16)

    tok_copy.wait_send()
    for c in range(chunks):
        part_copy(c).wait_send()

    @pl.when(me + 1 < sp_size)
    def _():
        halo_copy.wait_send()

    for step in range(1, sp_size):
        @pl.when(me + step < sp_size)
        def _():
            kv_copy(step).wait_send()
            carry_copy(step, me).wait_send()


def body(sp_size, tp_size, *args):
    (tokens, norm_gain, w_recur_in, conv_weight, w_gate_decay, w_gate_input, decay_base,
     extra_decay, w_query, w_key, w_value, mix_lambda, head_gain, w_out_recur, w_out_attend,
     out_gain) = args
    rows, half = tokens.shape
    width = w_recur_in.shape[0]
    recur_cols, query_cols = w_recur_in.shape[1], w_query.shape[1]
    kv_cols = w_key.shape[1] + w_value.shape[1]
    heads = query_cols // PAIR
    pairs = recur_cols // PAIR
    out_width = w_out_recur.shape[1]
    chunk = min(512, out_width)
    chunks = out_width // chunk
    own_rows = rows // tp_size
    halo = 16
    line = lambda a: a.reshape(1, -1)
    operands = (tokens, line(norm_gain), w_recur_in, conv_weight, w_gate_decay, w_gate_input,
                line(decay_base), extra_decay.T, w_query, w_key, w_value, line(mix_lambda),
                line(head_gain), w_out_recur, w_out_attend, line(out_gain))
    anywhere = pl.BlockSpec(memory_space=pl.ANY)
    specs = [anywhere] * len(operands)
    specs[11] = pl.BlockSpec(memory_space=pltpu.SMEM)
    like = lambda a: pltpu.VMEM(a.shape, a.dtype)
    dma = lambda n: pltpu.SemaphoreType.DMA((n,))
    return pl.pallas_call(
        functools.partial(kernel, sp_size, tp_size, conv_weight.shape[0]),
        out_shape=pltpu.VMEM((own_rows, out_width), BF16),
        in_specs=specs,
        out_specs=pl.BlockSpec(memory_space=pltpu.VMEM),
        scratch_shapes=[
            pltpu.VMEM((tp_size, rows, half), BF16),
            pltpu.VMEM((tp_size, rows, half), BF16),
            pltpu.VMEM((width, kv_cols), BF16),
            like(w_recur_in),
            like(w_query),
            like(w_out_recur),
            like(w_out_attend),
            like(operands[1]),
            like(conv_weight),
            like(w_gate_decay),
            like(w_gate_input),
            like(operands[6]),
            like(operands[7]),
            like(operands[12]),
            like(operands[15]),
            pltpu.VMEM((pairs, PAIR, 2 * PAIR), BF16),
            pltpu.VMEM((rows, kv_cols), F32),
            pltpu.VMEM((rows, recur_cols), F32),
            pltpu.VMEM((rows, query_cols), F32),
            pltpu.VMEM((sp_size, rows, kv_cols), BF16),
            pltpu.VMEM((halo + rows, recur_cols), BF16),
            pltpu.VMEM((heads, rows, PAIR), BF16),
            pltpu.VMEM((heads, 2, rows, PAIR), F32),
            pltpu.VMEM((heads, 2, rows, PAIR), F32),
            pltpu.VMEM((heads, 2, rows, PAIR), F32),
            pltpu.VMEM((rows, recur_cols), F32),
            pltpu.VMEM((rows, recur_cols), F32),
            pltpu.VMEM((2, recur_cols), F32),
            pltpu.VMEM((sp_size, 2, recur_cols), F32),
            pltpu.VMEM((1, recur_cols), F32),
            pltpu.VMEM((rows, query_cols), BF16),
            pltpu.VMEM((rows, out_width), F32),
            pltpu.VMEM((chunks, own_rows, chunk), BF16),
            pltpu.VMEM((chunks, own_rows, chunk), BF16),
            dma(19),
            dma(2),
            dma(sp_size),
            dma(sp_size),
            dma(2),
            dma(sp_size),
            dma(sp_size),
            dma(chunks),
            dma(chunks),
        ],
        compiler_params=pltpu.CompilerParams(collective_id=0, has_side_effects=True),
        name="layer",
    )(*operands)


def solution(mesh):
    in_specs = (
        P(("fs", "sp"), "tp"),
        P(),
        P(None, "tp"),
        P(None, "tp"),
        P("tp", None, None),
        P("tp", None, None),
        P("tp"),
        P(("fs", "sp"), "tp"),
        P(None, "tp"),
        P(None, "tp"),
        P(None, "tp"),
        P("tp"),
        P(),
        P("tp", None),
        P("tp", None),
        P(),
    )
    out_specs = P(("fs", "sp", "tp"), None)
    return jax.shard_map(
        functools.partial(body, mesh.shape["sp"], mesh.shape["tp"]),
        mesh=mesh, in_specs=in_specs, out_specs=out_specs, check_vma=False,
    )
```

```python
import functools

import jax
import jax.numpy as jnp
from jax import lax
from jax.experimental import pallas as pl
from jax.experimental.pallas import tpu as pltpu
from jax.sharding import PartitionSpec as P

HEAD = 64
PAIR = 2 * HEAD
MESH = pl.DeviceIdType.MESH
F32 = jnp.float32
BF16 = jnp.bfloat16

lru_rate = 8.0
norm_eps = 1e-06


def dot(a, b):
    return jnp.dot(a, b, preferred_element_type=F32)


def minus_expm1(y):
    series = 1.0 + y * (1.0 / 6.0)
    for k in (5.0, 4.0, 3.0, 2.0):
        series = 1.0 + y * (1.0 / k) * series
    return jnp.where(y > -0.25, -y * series, 1.0 - jnp.exp(y))


def kernel(
    sp_size,
    tp_size,
    taps,
    tokens,
    norm_gain,
    w_recur_in,
    conv_weight,
    w_gate_decay,
    w_gate_input,
    decay_base,
    extra_decay,
    w_query,
    w_key,
    w_value,
    mix_lambda,
    head_gain,
    w_out_recur,
    w_out_attend,
    out_gain,
    out,
    tok,
    scaled,
    wkv,
    wr,
    wq,
    wor,
    woa,
    v_norm_gain,
    v_conv,
    v_gate_decay,
    v_gate_input,
    v_base,
    v_extra,
    v_head_gain,
    v_out_gain,
    gates,
    acc_kv,
    acc_r,
    kv,
    rbuf,
    qbuf,
    peaks,
    totals,
    attends,
    cum_decay,
    local_state,
    carry_out,
    carry_in,
    carried,
    attend_out,
    merged,
    kept,
    part_out,
    part_in,
    load_sem,
    tok_sem,
    kv_send,
    kv_recv,
    halo_sem,
    carry_send,
    carry_recv,
    part_send,
    part_recv,
):
    me = lax.axis_index("sp")
    core = lax.axis_index("tp")
    partner = 1 - core
    rows, half = tokens.shape
    width = half * tp_size
    recur_cols = wr.shape[1]
    key_cols = w_key.shape[1]
    query_cols = wq.shape[1]
    kv_local = key_cols // PAIR
    heads = query_cols // PAIR
    group = heads // kv_local
    halo = rbuf.shape[0] - rows
    own_rows = rows // tp_size
    chunks, _, chunk = part_out.shape

    barrier = pltpu.get_barrier_semaphore()
    pl.semaphore_signal(barrier, inc=1, device_id={"tp": partner}, device_id_type=MESH)
    for step in range(1, sp_size):
        other = lax.rem(me + step, sp_size)
        pl.semaphore_signal(barrier, inc=1, device_id={"sp": other}, device_id_type=MESH)

    mine = pl.ds(pl.multiple_of(core * half, half), half)
    theirs = pl.ds(pl.multiple_of(partner * half, half), half)
    plan = {}

    def load(name, src, dst):
        copy = pltpu.make_async_copy(src, dst, load_sem.at[len(plan)])
        copy.start()
        plan[name] = copy

    load("tok", tokens, tok.at[core])
    load("norm_gain", norm_gain, v_norm_gain)
    load("r0", w_recur_in.at[mine], wr.at[mine])
    load("k0", w_key.at[mine], wkv.at[mine, pl.ds(0, key_cols)])
    load("v0", w_value.at[mine], wkv.at[mine, pl.ds(key_cols, wkv.shape[1] - key_cols)])
    load("r1", w_recur_in.at[theirs], wr.at[theirs])
    load("k1", w_key.at[theirs], wkv.at[theirs, pl.ds(0, key_cols)])
    load("v1", w_value.at[theirs], wkv.at[theirs, pl.ds(key_cols, wkv.shape[1] - key_cols)])

    pl.semaphore_wait(barrier, sp_size)
    plan["tok"].wait()
    tok_copy = pltpu.make_async_remote_copy(
        tok.at[core], tok.at[core], tok_sem.at[0], tok_sem.at[1],
        device_id={"tp": partner}, device_id_type=MESH,
    )
    tok_copy.start()

    def scale(part, columns):
        wide = tok[part].astype(F32)
        scaled[part] = (wide * v_norm_gain[:, columns]).astype(BF16)
        return jnp.sum(wide * wide, axis=1, keepdims=True)

    load("q0", w_query.at[mine], wq.at[mine])
    load("q1", w_query.at[theirs], wq.at[theirs])
    plan["norm_gain"].wait()
    squares = scale(core, mine)
    own = scaled[core]
    plan["r0"].wait()
    acc_r[...] = dot(own, wr[mine, :])
    plan["k0"].wait()
    plan["v0"].wait()
    acc_kv[...] = dot(own, wkv[mine, :])

    load("gate_decay", w_gate_decay, v_gate_decay)
    load("gate_input", w_gate_input, v_gate_input)
    load("conv", conv_weight, v_conv)
    load("base", decay_base, v_base)
    load("extra", extra_decay, v_extra)
    load("head_gain", head_gain, v_head_gain)
    load("out_gain", out_gain, v_out_gain)
    load("wor", w_out_recur, wor)
    load("woa", w_out_attend, woa)
    tok_copy.wait_recv()
    squares = squares + scale(partner, theirs)
    inverse = lax.rsqrt(squares / width + norm_eps)
    far = scaled[partner]
    plan["r1"].wait()
    rbuf[pl.ds(halo, rows), :] = ((acc_r[...] + dot(far, wr[theirs, :])) * inverse).astype(BF16)
    halo_copy = pltpu.make_async_remote_copy(
        rbuf.at[pl.ds(rows, halo)], rbuf.at[pl.ds(0, halo)], halo_sem.at[0], halo_sem.at[1],
        device_id={"sp": lax.rem(me + 1, sp_size)}, device_id_type=MESH,
    )

    @pl.when(me + 1 < sp_size)
    def _():
        halo_copy.start()

    @pl.when(me == 0)
    def _():
        rbuf[pl.ds(0, halo), :] = jnp.zeros((halo, recur_cols), BF16)

    plan["k1"].wait()
    plan["v1"].wait()
    kv[me] = ((acc_kv[...] + dot(far, wkv[theirs, :])) * inverse).astype(BF16)

    def kv_copy(step):
        return pltpu.make_async_remote_copy(
            kv.at[me], kv.at[me], kv_send.at[step], kv_recv.at[step],
            device_id={"sp": lax.rem(me + step, sp_size)}, device_id_type=MESH,
        )

    def direct(step):
        return (me + step < sp_size) & ((me == 0) | (step != 2))

    def relay():
        slot = kv.at[me - 1]
        return pltpu.make_async_remote_copy(
            slot, slot, kv_send.at[0], kv_recv.at[2],
            device_id={"sp": lax.rem(me + 1, sp_size)}, device_id_type=MESH,
        )

    relays = (me >= 2) & (me + 1 < sp_size)

    def kv_arrival(step):
        slot = kv.at[me - step]
        return pltpu.make_async_remote_copy(
            slot, slot, kv_send.at[step], kv_recv.at[step],
            device_id={"sp": lax.rem(me + step, sp_size)}, device_id_type=MESH,
        )

    for step in range(1, sp_size):
        @pl.when(direct(step) & ((me > 0) | (step in (1, sp_size - 1))))
        def _():
            kv_copy(step).start()

    plan["q0"].wait()
    plan["q1"].wait()
    query = (dot(own, wq[mine, :]) + dot(far, wq[theirs, :])) * (inverse * HEAD ** (-0.5))
    for h in range(heads):
        qbuf[h] = query[:, h * PAIR : (h + 1) * PAIR].astype(BF16)

    lane = lax.broadcasted_iota(jnp.int32, (rows, PAIR), 1)
    row = lax.broadcasted_iota(jnp.int32, (rows, PAIR), 0)
    low = lane < HEAD

    def attend(block, first):
        for g in range(kv_local):
            keys = kv[block, :, g * PAIR : (g + 1) * PAIR].astype(F32)
            value = kv[block, :, key_cols + g * PAIR : key_cols + (g + 1) * PAIR]
            both = jnp.concatenate(
                [jnp.where(low, keys, 0.0).astype(BF16), jnp.where(low, 0.0, keys).astype(BF16)], 0
            )
            for h in range(g * group, (g + 1) * group):
                scores = lax.dot_general(
                    qbuf[h], both, (((1,), (1,)), ((), ())), preferred_element_type=F32
                )
                for m in range(2):
                    score = scores[:, m * rows : (m + 1) * rows]
                    if first:
                        score = jnp.where(row >= lane, score, -jnp.inf)
                    top = jnp.broadcast_to(jnp.max(score, axis=1, keepdims=True), score.shape)
                    if first:
                        peak = top
                        expo = jnp.exp(score - peak)
                        totals[h, m] = expo
                        attends[h, m] = dot(expo.astype(BF16), value)
                    else:
                        before = peaks[h, m]
                        peak = jnp.maximum(before, top)
                        fix = jnp.exp(before - peak)
                        expo = jnp.exp(score - peak)
                        totals[h, m] = totals[h, m] * fix + expo
                        attends[h, m] = attends[h, m] * fix + dot(expo.astype(BF16), value)
                    peaks[h, m] = peak

    @pl.when(me > 0)
    def _():
        attend(me, True)

    plan["gate_decay"].wait()
    plan["gate_input"].wait()
    blank = jnp.zeros((HEAD, HEAD), F32)
    pairs = gates.shape[0]
    for p in range(pairs):
        for column, source in enumerate((v_gate_decay, v_gate_input)):
            upper = jnp.concatenate([source[2 * p].astype(F32), blank], 1)
            lower = jnp.concatenate([blank, source[2 * p + 1].astype(F32)], 1)
            gates[p, :, column * PAIR : (column + 1) * PAIR] = jnp.concatenate(
                [upper, lower], 0
            ).astype(BF16)

    for name in ("conv", "base", "extra"):
        plan[name].wait()

    @pl.when(me > 0)
    def _():
        halo_copy.wait_recv()

    start = halo - (taps - 1)
    spread = v_extra[...].T
    for p in range(pairs):
        columns = slice(p * PAIR, (p + 1) * PAIR)
        padded = rbuf[:, columns].astype(F32)
        conv = jnp.zeros((rows, PAIR), F32)
        for k in range(taps):
            conv = conv + v_conv[k : k + 1, columns] * padded[start + k : start + k + rows]
        conv_in = conv.astype(BF16)
        logits = dot(conv_in, gates[p])
        decay_gate = jax.nn.sigmoid(logits[:, :PAIR])
        input_gate = jax.nn.sigmoid(logits[:, PAIR:])
        extra = jnp.where(
            low,
            jnp.broadcast_to(spread[:, 2 * p : 2 * p + 1], (rows, PAIR)),
            jnp.broadcast_to(spread[:, 2 * p + 1 : 2 * p + 2], (rows, PAIR)),
        )
        log_decay = -lru_rate * decay_gate * v_base[:, columns] - extra
        decay = jnp.exp(log_decay)
        state = jnp.sqrt(minus_expm1(2.0 * log_decay)) * input_gate * conv_in.astype(F32)
        reach = 1
        while reach < rows:
            if reach < 8:
                earlier = row >= reach
                decay_before = jnp.where(earlier, pltpu.roll(decay, reach, 0), 1.0)
                state_before = jnp.where(earlier, pltpu.roll(state, reach, 0), 0.0)
            else:
                decay_before = jnp.concatenate(
                    [jnp.ones((reach, PAIR), F32), decay[: rows - reach]], 0
                )
                state_before = jnp.concatenate(
                    [jnp.zeros((reach, PAIR), F32), state[: rows - reach]], 0
                )
            state = decay * state_before + state
            decay = decay * decay_before
            reach *= 2
        cum_decay[:, columns] = decay
        local_state[:, columns] = state
        carry_out[0:1, columns] = decay[rows - 1 :]
        carry_out[1:2, columns] = state[rows - 1 :]

    def carry_copy(step, slot):
        return pltpu.make_async_remote_copy(
            carry_out, carry_in.at[slot], carry_send.at[step], carry_recv.at[step],
            device_id={"sp": lax.rem(me + step, sp_size)}, device_id_type=MESH,
        )

    for step in range(1, sp_size):
        @pl.when(me + step < sp_size)
        def _():
            carry_copy(step, me).start()

    @pl.when(me == 0)
    def _():
        for step in range(2, sp_size - 1):
            kv_copy(step).start()
        attend(me, True)

    def one(step, unused):
        kv_arrival(step).wait_recv()

        @pl.when(relays & (step == 1))
        def _():
            relay().start()

        attend(me - step, False)
        return unused

    lax.fori_loop(1, me, lambda k, unused: one(jnp.where(k == 1, 1, k + 1), unused), 0)

    carried[...] = jnp.zeros_like(carried)

    def link(back, unused):
        step = me - back
        carry_copy(step, back).wait_recv()
        carried[...] = carry_in[back, 0:1] * carried[...] + carry_in[back, 1:2]
        return unused

    lax.fori_loop(0, me, link, 0)
    recur_out = (local_state[...] + cum_decay[...] * carried[...]).astype(BF16)
    plan["wor"].wait()
    for c in range(chunks):
        columns = slice(c * chunk, (c + 1) * chunk)
        merged[:, columns] = dot(recur_out, wor[:, columns])

    last = jnp.minimum(me, 2)
    lax.fori_loop(jnp.maximum(last, 1), last + 1, one, 0)

    plan["head_gain"].wait()
    for h in range(heads):
        first, second = (
            attends[h, m] / jnp.sum(totals[h, m], axis=1, keepdims=True) for m in range(2)
        )
        head_out = first - mix_lambda[0, h] * second
        normed = (
            head_out
            * lax.rsqrt(jnp.mean(head_out * head_out, axis=1, keepdims=True) + norm_eps)
            * v_head_gain[...]
        )
        attend_out[:, h * PAIR : (h + 1) * PAIR] = normed.astype(BF16)

    plan["woa"].wait()
    attended = attend_out[...]

    def part_copy(c):
        return pltpu.make_async_remote_copy(
            part_out.at[c], part_in.at[c], part_send.at[c], part_recv.at[c],
            device_id={"tp": partner}, device_id_type=MESH,
        )

    for c in range(chunks):
        columns = slice(c * chunk, (c + 1) * chunk)
        both = merged[:, columns] + dot(attended, woa[:, columns])
        upper, lower = both[:own_rows], both[own_rows:]
        part_out[c] = jnp.where(core == 0, lower, upper).astype(BF16)
        part_copy(c).start()
        kept[:, columns] = jnp.where(core == 0, upper, lower)

    plan["out_gain"].wait()
    squares = jnp.zeros((own_rows, 1), F32)
    for c in range(chunks):
        columns = slice(c * chunk, (c + 1) * chunk)
        part_copy(c).wait_recv()
        whole = kept[:, columns] + part_in[c].astype(F32)
        kept[:, columns] = whole
        squares = squares + jnp.sum(whole * whole, axis=1, keepdims=True)
    final = lax.rsqrt(squares / out.shape[1] + norm_eps)
    for c in range(chunks):
        columns = slice(c * chunk, (c + 1) * chunk)
        out[:, columns] = (kept[:, columns] * final * v_out_gain[:, columns]).astype(BF16)

    tok_copy.wait_send()
    for c in range(chunks):
        part_copy(c).wait_send()

    @pl.when(me + 1 < sp_size)
    def _():
        halo_copy.wait_send()

    for step in range(1, sp_size):
        @pl.when(direct(step))
        def _():
            kv_copy(step).wait_send()

        @pl.when(me + step < sp_size)
        def _():
            carry_copy(step, me).wait_send()

    @pl.when(relays)
    def _():
        relay().wait_send()


def body(sp_size, tp_size, *args):
    (tokens, norm_gain, w_recur_in, conv_weight, w_gate_decay, w_gate_input, decay_base,
     extra_decay, w_query, w_key, w_value, mix_lambda, head_gain, w_out_recur, w_out_attend,
     out_gain) = args
    rows, half = tokens.shape
    width = w_recur_in.shape[0]
    recur_cols, query_cols = w_recur_in.shape[1], w_query.shape[1]
    kv_cols = w_key.shape[1] + w_value.shape[1]
    heads = query_cols // PAIR
    pairs = recur_cols // PAIR
    out_width = w_out_recur.shape[1]
    chunk = min(512, out_width)
    chunks = out_width // chunk
    own_rows = rows // tp_size
    halo = 16
    line = lambda a: a.reshape(1, -1)
    operands = (tokens, line(norm_gain), w_recur_in, conv_weight, w_gate_decay, w_gate_input,
                line(decay_base), extra_decay.T, w_query, w_key, w_value, line(mix_lambda),
                line(head_gain), w_out_recur, w_out_attend, line(out_gain))
    anywhere = pl.BlockSpec(memory_space=pl.ANY)
    specs = [anywhere] * len(operands)
    specs[11] = pl.BlockSpec(memory_space=pltpu.SMEM)
    like = lambda a: pltpu.VMEM(a.shape, a.dtype)
    dma = lambda n: pltpu.SemaphoreType.DMA((n,))
    return pl.pallas_call(
        functools.partial(kernel, sp_size, tp_size, conv_weight.shape[0]),
        out_shape=pltpu.VMEM((own_rows, out_width), BF16),
        in_specs=specs,
        out_specs=pl.BlockSpec(memory_space=pltpu.VMEM),
        scratch_shapes=[
            pltpu.VMEM((tp_size, rows, half), BF16),
            pltpu.VMEM((tp_size, rows, half), BF16),
            pltpu.VMEM((width, kv_cols), BF16),
            like(w_recur_in),
            like(w_query),
            like(w_out_recur),
            like(w_out_attend),
            like(operands[1]),
            like(conv_weight),
            like(w_gate_decay),
            like(w_gate_input),
            like(operands[6]),
            like(operands[7]),
            like(operands[12]),
            like(operands[15]),
            pltpu.VMEM((pairs, PAIR, 2 * PAIR), BF16),
            pltpu.VMEM((rows, kv_cols), F32),
            pltpu.VMEM((rows, recur_cols), F32),
            pltpu.VMEM((sp_size, rows, kv_cols), BF16),
            pltpu.VMEM((halo + rows, recur_cols), BF16),
            pltpu.VMEM((heads, rows, PAIR), BF16),
            pltpu.VMEM((heads, 2, rows, PAIR), F32),
            pltpu.VMEM((heads, 2, rows, PAIR), F32),
            pltpu.VMEM((heads, 2, rows, PAIR), F32),
            pltpu.VMEM((rows, recur_cols), F32),
            pltpu.VMEM((rows, recur_cols), F32),
            pltpu.VMEM((2, recur_cols), F32),
            pltpu.VMEM((sp_size, 2, recur_cols), F32),
            pltpu.VMEM((1, recur_cols), F32),
            pltpu.VMEM((rows, query_cols), BF16),
            pltpu.VMEM((rows, out_width), F32),
            pltpu.VMEM((own_rows, out_width), F32),
            pltpu.VMEM((chunks, own_rows, chunk), BF16),
            pltpu.VMEM((chunks, own_rows, chunk), BF16),
            dma(19),
            dma(2),
            dma(sp_size),
            dma(sp_size),
            dma(2),
            dma(sp_size),
            dma(sp_size),
            dma(chunks),
            dma(chunks),
        ],
        compiler_params=pltpu.CompilerParams(collective_id=0, has_side_effects=True),
        name="layer",
    )(*operands)


def solution(mesh):
    in_specs = (
        P(("fs", "sp"), "tp"),
        P(),
        P(None, "tp"),
        P(None, "tp"),
        P("tp", None, None),
        P("tp", None, None),
        P("tp"),
        P(("fs", "sp"), "tp"),
        P(None, "tp"),
        P(None, "tp"),
        P(None, "tp"),
        P("tp"),
        P(),
        P("tp", None),
        P("tp", None),
        P(),
    )
    out_specs = P(("fs", "sp", "tp"), None)
    return jax.shard_map(
        functools.partial(body, mesh.shape["sp"], mesh.shape["tp"]),
        mesh=mesh, in_specs=in_specs, out_specs=out_specs, check_vma=False,
    )
```
